512 devices in a mesh: ep: 32 (over z, core), tp: 16 (over y, x).
Axes of the slice: x: 4, y: 4, z: 16, core: 2. Of those that a mesh axis runs over, the one named last changes fastest.
Arguments:
- query_in: bfloat16 [1024, 32768], P('tp', 'ep'), may hold values from -6 to 6
- key_in: bfloat16 [1024, 32768], P('tp', 'ep'), may hold values from -10 to 10
- value_in: bfloat16 [1024, 32768], P('tp', 'ep'), may hold values from -6 to 6
- erase_pre: bfloat16 [1024, 32768], P('tp', 'ep'), may hold values from -8 to 5
- decay_pre: bfloat16 [1024, 32768], P('tp', 'ep'), may hold values from -30 to 4.5
- mix_gain: float32 [1024], P('tp'), may hold values from 0.1 to 1.9
- expert_in: bfloat16 [8192, 2048], P('ep'), may hold values from -6 to 6
- expert_gain: float32 [2048], replicated, may hold values from 0.1 to 1.9
- routes: int32 [8192, 2], P('ep'), may hold values from 0 to 31, all different within a row; in each aligned block of 256 rows (0 to 255, 256 to 511, ...) at most 24 rows name the same one
- route_weight: float32 [8192, 2], P('ep'), may hold values from 0.1 to 1
- gate_weight: bfloat16 [32, 2048, 3584], P('ep', None, 'tp'), may hold values from -0.125 to 0.125
- up_weight: bfloat16 [32, 2048, 3584], P('ep', None, 'tp'), may hold values from -0.125 to 0.125
- down_weight: bfloat16 [32, 3584, 2048], P('ep', 'tp'), may hold values from -0.09375 to 0.09375
Outputs:
- mixer_out: bfloat16 [1024, 32768], P('tp', 'ep')
- expert_out: bfloat16 [8192, 2048], P('ep', 'tp')
The draws below stay inside these ranges and needn't reach their ends.
Inputs may be any that keep to these rules, and one draw needn't show every extreme that they name: `routes`: A row's 2 experts differ. Within the 256 rows of one index of ep, every expert is named at most 24 times; in some of these aligned blocks one expert is named exactly 24 times.
All inputs are finite; a program needn't handle non-finite values.
Results may differ from the reference program's by a relative error of at most 0.015.
Values may be sent and summed in bfloat16 or wider, within the bound.
A program may use at most 64 MiB of HBM per device.

```python
import math
import jax
import jax.numpy as jnp
import numpy as np
from jax import lax

D = 2048
HEADS = 16
HEAD_DIM = 64
WIDTH = 1024
FFX = 3584
TOPK = 2
BLOCK_TOKENS = 64
TOK_EP = 256
SEQ_DEV = 1024
EXPERTS = 32
CAP = 24
TOKENS = 8192
SEQUENCE_LENGTH = 32768
N_EP = 32
N_TP = 16


spike_count = 3


spike_total = 2


aligned_scale = 2.0


def head_classes(key):
    head_count = WIDTH // HEAD_DIM
    fast_count = head_count // 2
    order = jax.random.permutation(jax.random.fold_in(key, 101), head_count)
    return jnp.repeat(order < fast_count, HEAD_DIM)


def strong_cells(key):
    quick_decay_channels = head_classes(key)
    total_blocks = SEQUENCE_LENGTH // BLOCK_TOKENS
    selected_experts = jax.random.randint(jax.random.fold_in(key, 202), (spike_total,), 0, total_blocks)
    spike_token_rows = jnp.any((jnp.arange(SEQUENCE_LENGTH) // BLOCK_TOKENS)[:, None] == selected_experts[None, :], axis=1)
    return jnp.logical_or(quick_decay_channels[None, :], spike_token_rows[:, None])


def draw_key_in(key, part):
    random_keys = jax.random.split(jax.random.fold_in(key, 303), 3)
    strong = strong_cells(key)
    own_part = jnp.clip(jax.random.normal(random_keys[0], (SEQUENCE_LENGTH, WIDTH), jnp.float32), -4.0, 4.0)
    direction = jnp.clip(jax.random.normal(random_keys[1], (WIDTH,), jnp.float32), -3.0, 3.0)
    signs = (jax.random.randint(random_keys[2], (SEQUENCE_LENGTH,), 0, 2) * 2 - 1).astype(jnp.float32)
    shared = aligned_scale * signs[:, None] * direction[None, :]
    keys_drawn = jnp.where(strong, own_part + shared, own_part)
    return jnp.clip(keys_drawn, -10.0, 10.0).T.astype(jnp.bfloat16)


def draw_erase_pre(key, part):
    random_keys = jax.random.split(jax.random.fold_in(key, 404), 2)
    strong = strong_cells(key)
    high_value = jnp.clip(2.5 + 1.2 * jax.random.normal(random_keys[0], (SEQUENCE_LENGTH, WIDTH), jnp.float32), 0.5, 5.0)
    low_value = jnp.clip(-7.0 + 0.5 * jax.random.normal(random_keys[1], (SEQUENCE_LENGTH, WIDTH), jnp.float32), -8.0, -6.0)
    return jnp.where(strong, high_value, low_value).T.astype(jnp.bfloat16)


def draw_decay_pre(key, part):
    random_keys = jax.random.split(key, 7)
    slow_mask = jnp.logical_not(head_classes(key))
    slow_rate = jnp.log(1.0 / SEQUENCE_LENGTH) + jax.random.uniform(random_keys[1], (WIDTH,), jnp.float32, -1.0, 1.0)
    fast_rate = jax.random.uniform(random_keys[2], (WIDTH,), jnp.float32, jnp.log(1.0 / 100.0), jnp.log(1.0 / 30.0))
    base_rate = jnp.where(slow_mask, slow_rate, fast_rate)
    device_shift = jnp.repeat(jax.random.uniform(random_keys[3], (SEQUENCE_LENGTH // SEQ_DEV, 1), jnp.float32, -0.7, 0.7), SEQ_DEV, axis=0)
    jitter = jnp.clip(jax.random.normal(random_keys[4], (SEQUENCE_LENGTH, WIDTH), jnp.float32), -3.0, 3.0) * 0.6
    logarithm_rate = jnp.minimum(base_rate[None, :] + device_shift + jitter, -1.0)
    locations = jax.random.randint(random_keys[5], (spike_count,), 0, SEQUENCE_LENGTH)
    spike_rows = jnp.any(jnp.arange(SEQUENCE_LENGTH)[:, None] == locations[None, :], axis=1)
    dropped_share = jax.random.uniform(random_keys[6], (SEQUENCE_LENGTH, WIDTH), jnp.float32, 0.2, 0.45)
    spike_rate = jnp.log(-jnp.log(1.0 - dropped_share))
    logarithm_rate = jnp.where(spike_rows[:, None], spike_rate, logarithm_rate)
    return (-jnp.log(jnp.expm1(-logarithm_rate - 0.5))).T.astype(jnp.bfloat16)


def block_levels(key, extent, shards, low, top_value):
    level = 1.0
    for axis_at, parts in shards:
        heights = jax.random.uniform(jax.random.fold_in(jax.random.fold_in(key, 6), axis_at), (parts,), jnp.float32, low / len(shards), top_value / len(shards))
        level = level * jnp.repeat(jnp.exp(heights), extent[axis_at] // parts).reshape((-1,) + (1,) * (len(extent) - 1 - axis_at))
    return level


def shared_out(rng, own, number, rows, amount, top, most, lean):
    order = jax.random.permutation(rng, amount)
    crowded, usual = load_shares(amount, rows * top, most, lean, True), load_shares(amount, rows * top, most, lean, False)
    places = jnp.arange(amount)

    def named(sizes, rotation):
        used = int((sizes > 0).sum())
        fixed = max(1, used // 4)
        passed = fixed + (places - fixed + rotation * (used - fixed)) % max(1, amount - fixed)
        return jnp.zeros((amount,), jnp.int32).at[order[jnp.where(places < fixed, places, passed)]].set(jnp.asarray(sizes, jnp.int32))

    sizes = jnp.where(number % 4 == 0, named(crowded, number // 4), named(usual, number - number // 4 - 1))
    mixed = jax.random.permutation(jax.random.fold_in(own, 3), amount)
    giver, receiver = mixed[0:amount // 2 * 2:2], mixed[1:amount // 2 * 2:2]
    slack = jnp.minimum(sizes[giver] - 1, most - sizes[receiver]) // 2
    slack = jnp.where((giver == order[0]) | (receiver == order[0]) | (sizes[receiver] == 0), 0, jnp.maximum(slack, 0))
    passed = jax.random.randint(jax.random.fold_in(own, 4), (amount // 2,), 0, 1 << 20) % (slack + 1)
    sizes = sizes.at[giver].add(-passed).at[receiver].add(passed)
    members = jnp.searchsorted(jnp.cumsum(sizes), jnp.arange(rows * top), side="right").astype(jnp.int32)
    listing = members.reshape(top, rows).T
    listing = listing[jax.random.permutation(jax.random.fold_in(own, 1), rows)]
    rotation = jax.random.randint(jax.random.fold_in(own, 2), (rows, 1), 0, top)
    return jnp.take_along_axis(listing, (jnp.arange(top)[None, :] + rotation) % top, axis=1)


def load_shares(number_of, total, limit, slope, full):
    portions = [(1 << 20) // math.isqrt(rank ** slope) + 1 for rank in range(1, number_of + 1)]
    largest = limit if full else min(limit, max(-(-total // number_of), total * portions[0] // sum(portions)))
    least = 1 if total - largest >= number_of - 1 else 0
    given, spare = [largest] + [least] * (number_of - 1), total - largest - least * (number_of - 1)
    while spare > 0:
        free = [i for i in range(1, number_of) if given[i] < largest] or [i for i in range(1, number_of) if given[i] < limit]
        mass, budget = sum([portions[i] for i in free]), spare
        for i in free:
            more = min(limit - given[i], max(1, budget * portions[i] // mass), spare)
            given[i] = given[i] + more
            spare = spare - more
    return np.array(given)


def gaussian(stream_key, dims, width, bound, cuts=(), kind=jnp.bfloat16):
    values = width * jax.random.normal(stream_key, dims, jnp.float32)
    if cuts:
        values = values * block_levels(stream_key, dims, cuts, -0.22, 0.18)
    return jnp.clip(values, -bound, bound).astype(kind)


def setup_inputs(seed: int = 0) -> dict:
    streams_of = jax.random.split(jax.random.key(seed), 14)
    query_in = gaussian(streams_of[0], (WIDTH, SEQUENCE_LENGTH), 1.0, 6.0, ((0, 16), (1, 32)))
    key_in = draw_key_in(jax.random.fold_in(streams_of[13], 71), 0)
    value_in = gaussian(streams_of[2], (WIDTH, SEQUENCE_LENGTH), 1.0, 6.0, ((0, 16), (1, 32)))
    erase_pre = draw_erase_pre(jax.random.fold_in(streams_of[13], 71), 0)
    decay_pre = draw_decay_pre(jax.random.fold_in(streams_of[13], 71), 0)
    mix_gain = jnp.clip(1.0 + 0.18 * jax.random.normal(streams_of[5], (WIDTH,), jnp.float32), 0.1, 1.9)
    expert_in = gaussian(streams_of[6], (TOKENS, D), 1.0, 6.0, ((0, 32),))
    expert_gain = jnp.clip(1.0 + 0.18 * jax.random.normal(streams_of[7], (D,), jnp.float32), 0.1, 1.9)
    routes_keys = jax.random.split(jax.random.fold_in(streams_of[8], 1), TOKENS // TOK_EP)
    routes_turns = jax.random.permutation(jax.random.fold_in(streams_of[8], 3), TOKENS // TOK_EP)
    routes = jax.vmap(lambda own, number: shared_out(jax.random.fold_in(streams_of[8], 2), own, number, TOK_EP, EXPERTS, TOPK, CAP, 2))(routes_keys, routes_turns).reshape((TOKENS, TOPK))
    route_weight = jnp.clip(0.1 + 0.9 * jax.random.uniform(streams_of[9], (TOKENS, TOPK), jnp.float32) ** block_levels(streams_of[9], (TOKENS, TOPK), ((0, 32),), -0.2, 0.2), 0.1, 1.0)
    gate_weight = gaussian(streams_of[10], (EXPERTS, D, FFX), D ** -0.5, 0.125, ((0, 32), (2, 16)))
    up_weight = gaussian(streams_of[11], (EXPERTS, D, FFX), D ** -0.5, 0.125, ((0, 32), (2, 16)))
    down_weight = gaussian(streams_of[12], (EXPERTS, FFX, D), FFX ** -0.5, 0.09375, ((0, 32), (1, 16)))
    return {"query_in": query_in, "key_in": key_in, "value_in": value_in, "erase_pre": erase_pre, "decay_pre": decay_pre, "mix_gain": mix_gain, "expert_in": expert_in, "expert_gain": expert_gain, "routes": routes, "route_weight": route_weight, "gate_weight": gate_weight, "up_weight": up_weight, "down_weight": down_weight}


highest = lax.Precision.HIGHEST

def token_terms(key_in, erase_pre, decay_pre):
    key_f = key_in.astype(jnp.float32)
    unit_key = key_f * lax.rsqrt(lax.optimization_barrier(jnp.sum(key_f * key_f, axis=-1, keepdims=True)) + 1e-05)
    eraser = unit_key * jax.nn.sigmoid(erase_pre.astype(jnp.float32))
    log_keep = -jnp.exp(-jax.nn.softplus(-decay_pre.astype(jnp.float32)) - 0.5)
    return (key_f, unit_key, eraser, log_keep)

def advance(carried, inputs):
    query_f, key_f, value_f, unit_key, eraser, keep = inputs
    seen = jnp.einsum('hvk,hk->hv', carried, unit_key, precision=highest)
    carried = carried * keep[:, None, :] - seen[:, :, None] * eraser[:, None, :] + value_f[:, :, None] * key_f[:, None, :]
    return (carried, jnp.einsum('hvk,hk->hv', carried, query_f, precision=highest))

def mixer(query_in, key_in, value_in, erase_pre, decay_pre, mix_gain):
    layout = (SEQUENCE_LENGTH, HEADS, HEAD_DIM)
    query_f = query_in.astype(jnp.float32).reshape(layout)
    value_f = value_in.astype(jnp.float32).reshape(layout)
    key_f, unit_key, eraser, log_keep = token_terms(key_in.reshape(layout), erase_pre.reshape(layout), decay_pre.reshape(layout))
    inputs = (query_f, key_f, value_f, unit_key, eraser, jnp.exp(log_keep))
    initial = jnp.zeros((HEADS, HEAD_DIM, HEAD_DIM), jnp.float32)
    _, ahead = lax.scan(advance, initial, inputs)
    _, behind = lax.scan(advance, initial, inputs, reverse=True)
    summed = ahead + behind
    center = lax.optimization_barrier(jnp.mean(summed, axis=-1, keepdims=True))
    spread = lax.optimization_barrier(jnp.mean(jnp.square(summed - center), axis=-1, keepdims=True))
    scaled = (summed - center) * lax.rsqrt(spread + HEAD_DIM * 1e-05) * mix_gain.reshape(HEADS, HEAD_DIM)
    return scaled.astype(jnp.bfloat16).reshape(SEQUENCE_LENGTH, HEADS * HEAD_DIM)

def slot_targets(routes):
    onehot = (routes[:, :, None] == jnp.arange(EXPERTS, dtype=jnp.int32)[None, None, :]).astype(jnp.int32)
    flat = onehot.reshape(-1, EXPERTS)
    before = jnp.cumsum(flat, axis=0) - flat
    slot_index = lax.optimization_barrier(jnp.sum(before * flat, axis=-1)).reshape(routes.shape)
    return routes * CAP + slot_index

def dispatch_matrix(targets, slot_total):
    matches = targets[None, :, :] == jnp.arange(slot_total, dtype=jnp.int32)[:, None, None]
    return lax.optimization_barrier(jnp.sum(matches.astype(jnp.float32), axis=-1)).astype(jnp.bfloat16)

def experts_part(expert_in, expert_gain, routes, route_weight, gate_weight, up_weight, down_weight):
    input_f = expert_in.astype(jnp.float32)
    normed = (input_f * lax.rsqrt(lax.optimization_barrier(jnp.mean(input_f * input_f, axis=-1, keepdims=True)) + 1e-06) * expert_gain).astype(jnp.bfloat16)
    targets = jax.vmap(slot_targets)(routes.reshape(N_EP, TOK_EP, TOPK))

    def fill(pack):
        selected_experts, rows = pack
        return jnp.dot(dispatch_matrix(selected_experts, EXPERTS * CAP), rows, preferred_element_type=jnp.float32).astype(jnp.bfloat16)
    buffers = lax.map(fill, (targets, normed.reshape(N_EP, TOK_EP, D)))
    buffers = buffers.reshape(N_EP, EXPERTS, CAP, D).transpose(1, 0, 2, 3).reshape(EXPERTS, N_EP * CAP, D)

    def expert(pack):
        rows, gate_mat, up_mat, down_mat = pack
        gate_sum = jnp.dot(rows, gate_mat, preferred_element_type=jnp.float32)
        up_sum = jnp.dot(rows, up_mat, preferred_element_type=jnp.float32)
        hidden = (jax.nn.silu(gate_sum) * up_sum).astype(jnp.bfloat16)
        groups = hidden.reshape(-1, N_TP, FFX // N_TP).astype(jnp.float32)
        downs = down_mat.reshape(N_TP, FFX // N_TP, D).astype(jnp.float32)
        partial_value = jnp.einsum('rjf,jfd->jrd', groups, downs).astype(jnp.bfloat16)
        partial_value = lax.optimization_barrier(partial_value)
        return lax.optimization_barrier(jnp.sum(partial_value.astype(jnp.float32), axis=0)).astype(jnp.bfloat16)
    results = lax.map(expert, (buffers, gate_weight, up_weight, down_weight)).reshape(EXPERTS, N_EP, CAP, D)
    source = (jnp.arange(TOKENS, dtype=jnp.int32) // TOK_EP)[:, None]
    slot_index = targets.reshape(TOKENS, TOPK) - routes * CAP
    picked = results[routes, source, slot_index].astype(jnp.float32)
    return lax.optimization_barrier(jnp.sum(picked * route_weight[:, :, None], axis=1)).astype(jnp.bfloat16)

def reference(query_in, key_in, value_in, erase_pre, decay_pre, mix_gain, expert_in, expert_gain, routes, route_weight, gate_weight, up_weight, down_weight):
    mixer_out = mixer(query_in.T, key_in.T, value_in.T, erase_pre.T, decay_pre.T, mix_gain).T
    expert_out = experts_part(expert_in, expert_gain, routes, route_weight, gate_weight, up_weight, down_weight)
    return (mixer_out, expert_out)
```

```python
import jax
import jax.numpy as jnp
from jax import lax
from jax.experimental import pallas as pl
from jax.experimental.pallas import tpu as pltpu
from jax.sharding import PartitionSpec as P

HEAD_DIM = 64
SPAN = 128
BF = jnp.bfloat16
F32 = jnp.float32
NN = (((1,), (0,)), ((), ()))
TN = (((0,), (0,)), ((), ()))
NT = (((1,), (1,)), ((), ()))


def dot(a, b, dims=NN):
    return lax.dot_general(a, b, dims, preferred_element_type=F32)


def halves(a):
    high = a.astype(BF)
    return high, (a - high.astype(F32)).astype(BF)


def dot_tn(a, b):
    ah, al = halves(a)
    bh, bl = halves(b)
    return dot(jnp.concatenate([ah, al, ah], 0), jnp.concatenate([bh, bh, bl], 0), TN)


def dot_wide(a, b):
    width = b.shape[1]
    ah, al = halves(a)
    bh, bl = halves(b)
    right = jnp.concatenate(
        [jnp.concatenate([bh, bl], 1), jnp.concatenate([bh, jnp.zeros_like(bh)], 1)], 0
    )
    both = dot(jnp.concatenate([ah, al], 1), right)
    return both[:, :width] + both[:, width:]


def dot_nt(a, b):
    ah, al = halves(a)
    bh, bl = halves(b)
    return dot(jnp.concatenate([ah, al], 1), jnp.concatenate([bh, bh], 1), NT) + dot(ah, bl, NT)


def exact_left(a, b):
    width = b.shape[1]
    bh, bl = halves(b)
    both = dot(a, jnp.concatenate([bh, bl], 1))
    return both[:, :width] + both[:, width:]


def unit_inverses(lowers, row, col):
    span = row.shape[0]
    found = [
        jnp.where(row == col, 1.0, 0.0) - jnp.where(row // 2 == col // 2, low, 0.0)
        for low in lowers
    ]
    size = 2
    while size < span:
        cross = (row // (2 * size) == col // (2 * size)) & (row // size != col // size)
        cut = [jnp.where(cross, low, 0.0) for low in lowers]
        cut = [dot_wide(c, x) for c, x in zip(cut, found)]
        found = [x - dot_wide(x, c) for c, x in zip(cut, found)]
        size *= 2
    return found


def mixer_group(starts, refs, abt_ref, pt_ref, ol_ref):
    query_ref, key_ref, value_ref, erase_ref, decay_ref = refs
    row = lax.broadcasted_iota(jnp.int32, (SPAN, SPAN), 0)
    col = lax.broadcasted_iota(jnp.int32, (SPAN, SPAN), 1)
    tri = (row <= col).astype(BF)
    head_row = lax.broadcasted_iota(jnp.int32, (HEAD_DIM, 2 * HEAD_DIM), 0)
    head_col = lax.broadcasted_iota(jnp.int32, (HEAD_DIM, 2 * HEAD_DIM), 1)
    chains = []
    for start in starts:
        at = (slice(None), pl.ds(start * SPAN, SPAN))
        query = query_ref[at].astype(F32)
        key = key_ref[at].astype(F32)
        value = value_ref[at]
        erase = erase_ref[at].astype(F32)
        decay = decay_ref[at].astype(F32)
        unit = key * lax.rsqrt(jnp.sum(key * key, axis=0, keepdims=True) + 1e-05)
        eraser = unit / (1.0 + jnp.exp(-erase))
        log_keep = -jnp.exp(-0.5) / (1.0 + jnp.exp(-decay))
        high = log_keep.astype(BF)
        rest = log_keep - high.astype(F32)
        middle = rest.astype(BF)
        low = (rest - middle.astype(F32)).astype(BF)
        cumulative = dot(jnp.concatenate([high, middle, low], 1), jnp.concatenate([tri] * 3, 0))
        total = cumulative[:, SPAN - 1 : SPAN]
        for back in (False, True):
            through = total - cumulative + log_keep if back else cumulative
            prior = through - log_keep
            strict = row > col if back else row < col
            inclusive = row >= col if back else row <= col
            growth = jnp.exp(-through)
            fade = jnp.exp(total - through)
            chains.append(
                dict(
                    start=start,
                    back=back,
                    value=value,
                    strict=strict,
                    inclusive=inclusive,
                    left=jnp.concatenate([key * growth, eraser * growth], 1),
                    unit_down=unit * jnp.exp(prior),
                    query_down=query * jnp.exp(through),
                    key_end=key * fade,
                    erase_end=eraser * fade,
                    faded=jnp.where(head_row == head_col, jnp.exp(total), 0.0),
                )
            )
    for c in chains:
        pairs = dot_tn(c["left"], jnp.concatenate([c["unit_down"], c["query_down"]], 1))
        c["key_mix"] = jnp.where(c["strict"], pairs[:SPAN, :SPAN], 0.0)
        c["key_read"] = jnp.where(c["inclusive"], pairs[:SPAN, SPAN:], 0.0)
        c["erase_mix"] = jnp.where(c["strict"], pairs[SPAN:, :SPAN], 0.0)
        c["erase_read"] = jnp.where(c["inclusive"], pairs[SPAN:, SPAN:], 0.0)
    inverses = unit_inverses([c["erase_mix"] for c in chains], row, col)
    for c, inverse in zip(chains, inverses):
        seen = exact_left(c["value"], jnp.concatenate([c["key_mix"], c["key_read"]], 1))
        removed = dot_wide(jnp.concatenate([c["unit_down"], seen[:, :SPAN]], 0), inverse)
        read = jnp.concatenate([c["query_down"], seen[:, SPAN:]], 0) - dot_wide(
            removed, c["erase_read"]
        )
        ended = jnp.concatenate(
            [c["faded"][:, :HEAD_DIM], dot(jnp.concatenate(halves(c["key_end"]), 1), jnp.concatenate([c["value"]] * 2, 1), NT)], 1
        ) - dot_nt(c["erase_end"], removed)
        d = int(c["back"])
        abt_ref[d, c["start"]] = ended
        pt_ref[d, c["start"]] = read[:HEAD_DIM]
        ol_ref[d, c["start"]] = read[HEAD_DIM:]


def mixer_local(refs, abt_ref, pt_ref, ol_ref, group):
    blocks = refs[0].shape[1] // SPAN

    @pl.loop(0, blocks // group)
    def _(step):
        mixer_group([step * group + i for i in range(group)], refs, abt_ref, pt_ref, ol_ref)


def carry_maps(abt_ref, pt_ref, ol_ref, reach_ref):
    blocks = abt_ref.shape[1]
    row = lax.broadcasted_iota(jnp.int32, (HEAD_DIM, 2 * HEAD_DIM), 0)
    col = lax.broadcasted_iota(jnp.int32, (HEAD_DIM, 2 * HEAD_DIM), 1)
    first = jnp.where(row == col, 1.0, 0.0)
    tail = jnp.where(row + HEAD_DIM == col, 1.0, 0.0)

    def step(i, carried):
        after = []
        for d in (0, 1):
            at = blocks - 1 - i if d else i
            state = carried[d]
            both = dot_tn(state, pt_ref[d, at])
            reach_ref[d, :, pl.ds(at * SPAN, SPAN)] = both[:HEAD_DIM]
            ol_ref[d, at] = ol_ref[d, at] + both[HEAD_DIM:]
            after.append(dot_wide(abt_ref[d, at], jnp.concatenate([state, tail], 0)))
        return tuple(after)

    return lax.fori_loop(0, blocks, step, (first, first))


def mixer_finish(enter, ol_ref, reach_ref, gain_ref, out_ref):
    local = jnp.concatenate([ol_ref[0, b] + ol_ref[1, b] for b in range(ol_ref.shape[1])], 1)
    reach = jnp.concatenate([reach_ref[0], reach_ref[1]], 0)
    eh, el = halves(enter)
    rh, rl = halves(reach)
    summed = local + dot(jnp.concatenate([eh, el], 0), jnp.concatenate([rh, rh], 0), TN)
    summed = summed + dot(eh, rl, TN)
    center = jnp.mean(summed, axis=0, keepdims=True)
    spread = jnp.mean(jnp.square(summed - center), axis=0, keepdims=True)
    scaled = (summed - center) * lax.rsqrt(spread + HEAD_DIM * 1e-05) * gain_ref[...]
    out_ref[...] = scaled.astype(BF)


def sent_to_all(array, axis):
    count = lax.axis_size(axis)
    return lax.all_to_all(
        jnp.broadcast_to(array[None], (count, *array.shape)), axis, 0, 0, tiled=True
    )


def gathered_once(array, axis):
    leaves = jax.tree.leaves(array)
    sequence = sorted(range(len(leaves)), key=lambda k: -leaves[k].size)
    width = (1, *leaves[sequence[0]].shape)[-1]
    lines = [
        jnp.pad(leaves[k].reshape(-1), (0, -leaves[k].size % width)).reshape(-1, width)
        for k in sequence
    ]
    both, at, found = (sent_to_all(jnp.concatenate(lines), axis), 0, {})
    for k, line in zip(sequence, lines):
        section = both[:, at : at + len(line)].reshape(len(both), -1)
        found[k] = section[:, : leaves[k].size].reshape(-1, *leaves[k].shape)
        at += len(line)
    numbers = iter(range(len(leaves)))
    return jax.tree.map(lambda _: found[next(numbers)], array)


def combined_pairwise(pieces, combine):
    while len(jax.tree.leaves(pieces)[0]) > 1:
        pieces = jax.vmap(combine)(
            *(jax.tree.map(lambda part: part[side::2], pieces) for side in (0, 1))
        )
    return jax.tree.map(lambda part: part[0], pieces)


def prefix(array, axis, combine, identity, reverse):
    count, mine = (lax.axis_size(axis), lax.axis_index(axis))
    passed = jnp.arange(count) > mine if reverse else jnp.arange(count) < mine

    def kept(part, zero, own):
        part = jnp.where(
            passed.reshape(-1, *(1 for _ in own.shape)),
            part.astype(own.dtype),
            jnp.asarray(zero, own.dtype),
        )
        return part[::-1] if reverse else part

    pieces = gathered_once(
        jax.tree.map(
            lambda part, kind: part.astype(kind),
            array,
            jax.tree.map(lambda a: jnp.bfloat16 if a.dtype == jnp.float32 else a.dtype, array),
        ),
        axis,
    )
    return combined_pairwise(jax.tree.map(kept, pieces, identity, array), combine)


def in_blocks(array, dim, count):
    before, after = (array.shape[:dim], array.shape[dim + 1 :])
    return jnp.moveaxis(array.reshape(*before, count, -1, *after), dim, 0)


def summed_on_arrival(array, axis, dim):
    count = lax.axis_size(axis)
    parts = lax.all_to_all(in_blocks(array, dim, count), axis, 0, 0, tiled=True)
    return jnp.sum(parts.astype(jnp.float32), axis=0)


def compose(earlier, later):
    return (
        jnp.einsum("hij,hjk->hik", earlier[0], later[0]),
        jnp.einsum("hvj,hjk->hvk", earlier[1], later[0]) + later[1],
    )


def local_kernel(q, k, v, e, d, map_ref, ol_ref, reach_ref, abt_ref, pt_ref):
    mixer_local((q, k, v, e, d), abt_ref, pt_ref, ol_ref, 4)
    ahead, behind = carry_maps(abt_ref, pt_ref, ol_ref, reach_ref)
    map_ref[0] = ahead
    map_ref[1] = behind


def finish_kernel(enter_ref, ol_ref, reach_ref, gain_ref, out_ref):
    mixer_finish(enter_ref[...], ol_ref, reach_ref, gain_ref, out_ref)


def mixer_half(query_in, key_in, value_in, erase_pre, decay_pre, mix_gain):
    tokens = query_in.shape[1]
    blocks = tokens // SPAN
    maps, local, reach = pl.pallas_call(
        local_kernel,
        out_shape=(
            jax.ShapeDtypeStruct((2, HEAD_DIM, 2 * HEAD_DIM), F32),
            jax.ShapeDtypeStruct((2, blocks, HEAD_DIM, SPAN), F32),
            jax.ShapeDtypeStruct((2, HEAD_DIM, tokens), F32),
        ),
        scratch_shapes=[
            pltpu.VMEM((2, blocks, HEAD_DIM, 2 * HEAD_DIM), F32),
            pltpu.VMEM((2, blocks, HEAD_DIM, SPAN), F32),
        ],
        name="mixer_local",
    )(query_in, key_in, value_in, erase_pre, decay_pre)
    turned = jnp.swapaxes(maps, 1, 2)
    ahead_maps = (turned[:1, :HEAD_DIM], turned[:1, HEAD_DIM:])
    behind_maps = (turned[1:, :HEAD_DIM], turned[1:, HEAD_DIM:])
    empty_state = jnp.zeros((1, HEAD_DIM, HEAD_DIM), F32)
    identity_maps = (jnp.eye(HEAD_DIM, dtype=F32)[None], empty_state)
    enter_ahead = prefix(ahead_maps, "ep", compose, identity_maps, False)[1]
    enter_behind = prefix(behind_maps, "ep", compose, identity_maps, True)[1]
    enter = jnp.concatenate([enter_ahead[0].T, enter_behind[0].T], 0)
    return pl.pallas_call(
        finish_kernel,
        out_shape=jax.ShapeDtypeStruct(query_in.shape, BF),
        name="mixer_finish",
    )(enter, local, reach, mix_gain.reshape(-1, 1))


def slot_targets(routes, experts_n, capacity):
    onehot = (routes[:, :, None] == jnp.arange(experts_n, dtype=jnp.int32)[None, None, :]).astype(
        jnp.int32
    )
    flat = onehot.reshape(-1, experts_n)
    before = jnp.cumsum(flat, axis=0) - flat
    slot_index = jnp.sum(before * flat, axis=-1).reshape(routes.shape)
    return routes * capacity + slot_index


def dispatch_matrix(targets, slot_total):
    matches = targets[None, :, :] == jnp.arange(slot_total, dtype=jnp.int32)[:, None, None]
    return jnp.sum(matches.astype(jnp.float32), axis=-1).astype(jnp.bfloat16)


def expert_half(expert_in, expert_gain, routes, route_weight, gate_weight, up_weight, down_weight):
    experts_n = lax.axis_size("ep")
    row_count = expert_in.shape[0]
    capacity = 3 * routes.shape[1] * row_count // (2 * experts_n)
    slot_total = experts_n * capacity
    input_f = expert_in.astype(jnp.float32)
    normed = (
        input_f
        * lax.rsqrt(jnp.mean(input_f * input_f, axis=-1, keepdims=True) + 1e-06)
        * expert_gain
    ).astype(jnp.bfloat16)
    targets = slot_targets(routes, experts_n, capacity)
    buffer = jnp.dot(
        dispatch_matrix(targets, slot_total), normed, preferred_element_type=jnp.float32
    ).astype(jnp.bfloat16)
    gate_local = gate_weight[0]
    up_local = up_weight[0]
    down_local = down_weight[0]
    col_count = normed.shape[1] // lax.axis_size("tp")
    own_cols = lax.dynamic_slice_in_dim(buffer, lax.axis_index("tp") * col_count, col_count, 1)
    arrived = lax.all_to_all(
        own_cols.reshape(experts_n, capacity, col_count),
        "ep",
        split_axis=0,
        concat_axis=0,
        tiled=True,
    ).reshape(slot_total, col_count)
    portion = lax.all_gather(arrived, "tp", axis=1, tiled=True)
    gate_sum = jnp.dot(portion, gate_local, preferred_element_type=jnp.float32)
    up_sum = jnp.dot(portion, up_local, preferred_element_type=jnp.float32)
    hidden = (jax.nn.silu(gate_sum) * up_sum).astype(jnp.bfloat16)
    summed = summed_on_arrival(
        lax.dot_general(
            down_local, hidden, (((0,), (1,)), ((), ())), preferred_element_type=jnp.float32
        ).astype(jnp.bfloat16),
        "tp",
        0,
    ).astype(jnp.bfloat16)
    returned = lax.all_to_all(
        summed.reshape(col_count, experts_n, capacity),
        "ep",
        split_axis=1,
        concat_axis=1,
        tiled=True,
    ).reshape(col_count, slot_total)
    matches = targets[:, :, None] == jnp.arange(slot_total, dtype=jnp.int32)[None, None, :]
    combine = jnp.sum(matches.astype(jnp.float32) * route_weight[:, :, None], axis=1)
    return jnp.einsum("tx,cx->tc", combine, returned.astype(jnp.float32)).astype(jnp.bfloat16)


def on_device(
    query_in,
    key_in,
    value_in,
    erase_pre,
    decay_pre,
    mix_gain,
    expert_in,
    expert_gain,
    routes,
    route_weight,
    gate_weight,
    up_weight,
    down_weight,
):
    mixer_out = mixer_half(query_in, key_in, value_in, erase_pre, decay_pre, mix_gain)
    expert_out = expert_half(
        expert_in, expert_gain, routes, route_weight, gate_weight, up_weight, down_weight
    )
    return (mixer_out, expert_out)


def solution(mesh):
    placed = (
        P("tp", "ep"),
        P("tp", "ep"),
        P("tp", "ep"),
        P("tp", "ep"),
        P("tp", "ep"),
        P("tp"),
        P("ep", None),
        P(),
        P("ep", None),
        P("ep", None),
        P("ep", None, "tp"),
        P("ep", None, "tp"),
        P("ep", "tp", None),
    )
    return jax.shard_map(
        on_device,
        mesh=mesh,
        in_specs=placed,
        out_specs=(P("tp", "ep"), P("ep", "tp")),
        check_vma=False,
    )
```
